128 devices in a mesh: sp: 16 (over z, x), dp: 8 (over y, core).
Axes of the slice: x: 4, y: 4, z: 4, core: 2. Of those that a mesh axis runs over, the one named last changes fastest.
Arguments:
- queries: bfloat16 [8, 2048, 16, 128], P('dp', 'sp'), may hold values from -6 to 6
- key_rows: bfloat16 [8, 2048, 4, 128], P('dp', 'sp'), may hold values from -6 to 6
- values: bfloat16 [8, 2048, 4, 128], P('dp', 'sp'), may hold values from -6 to 6
- query_gain: float32 [128], replicated, may hold values from 0.4 to 5
- key_gain: float32 [128], replicated, may hold values from 0.4 to 5
- out_weight: bfloat16 [2048, 2048], P('sp', 'dp'), may hold values from -0.125 to 0.125
- residual: bfloat16 [8, 2048, 2048], P('dp', 'sp'), may hold values from -6 to 6
- norm_gain: float32 [2048], replicated, may hold values from 0.1 to 1.9
- expert_gate: bfloat16 [16, 2048, 1792], P('sp'), may hold values from -0.125 to 0.125
- expert_up: bfloat16 [16, 2048, 1792], P('sp'), may hold values from -0.125 to 0.125
- expert_down: bfloat16 [16, 1792, 2048], P('sp'), may hold values from -0.125 to 0.125
- routes: int32 [8, 2048, 2], P('dp', 'sp'), may hold values from 0 to 15, all different within a row; in each aligned block of 64 rows (0 to 63, 64 to 127, ..., all dimensions but the last counted through in order) at most 16 rows name the same one
- route_weight: float32 [8, 2048, 2], P('dp', 'sp'), may hold values from 0.25 to 1
Outputs:
- layer_out: bfloat16 [8, 2048, 2048], P('dp', 'sp')
The draws below stay inside these ranges and needn't reach their ends.
Inputs may be any that keep to these rules, and one draw needn't show every extreme that they name: `routes`: in each aligned block of 64 rows of one device, no expert is named by more than 16 entries, a bound that some block reaches; the two experts of a row differ.
All inputs are finite; a program needn't handle non-finite values.
Results may differ from the reference program's by a relative error of at most 0.0095.
The reference program's roundings to bfloat16 on the way count: a program that leaves them out, or rounds other values in their place, can miss the bound.
Values may be sent and summed in bfloat16 or wider, within the bound.
A program may use at most 128 MiB of HBM per device.

```python
import math
import jax
import jax.numpy as jnp
import numpy as np
from jax import lax

D = 2048
HEADS = 16
KV_HEADS = 4
HEAD_DIM = 128
EXPERT_FF = 1792
GRID_W = 64
SEQS = 8
LENGTH = 2048
EXPERTS = 16
HALF = 64
CAP = 16


def shared_keys(key):
    drawn = jax.random.normal(jax.random.fold_in(key, 11), (SEQS, LENGTH, KV_HEADS, HEAD_DIM), jnp.float32)
    return jnp.clip(drawn, -6.0, 6.0)


def draw_key_rows(key, part):
    return shared_keys(key).astype(jnp.bfloat16)


def draw_queries(key, part):
    drawn = jax.random.normal(jax.random.fold_in(key, 12), (SEQS, LENGTH, HEADS, HEAD_DIM), jnp.float32)
    drawn = jnp.clip(drawn, -6.0, 6.0)
    return drawn.astype(jnp.bfloat16)


def gain_draw(key, salt):
    drawn = jax.random.normal(jax.random.fold_in(key, salt), (HEAD_DIM,), jnp.float32)
    return 1.0 + 0.18 * jnp.clip(drawn, -3.0, 3.0)


def draw_query_gain(key, part):
    return gain_draw(key, 21)


def draw_key_gain(key, part):
    return gain_draw(key, 22)


def block_levels(stream_key, extent, pieces, low, top_value):
    def one(dim, parts):
        heights = jax.random.uniform(jax.random.fold_in(jax.random.fold_in(stream_key, 6), dim), (parts,), jnp.float32, low / len(pieces), top_value / len(pieces))
        return jnp.repeat(jnp.exp(heights), extent[dim] // parts).reshape((-1,) + (1,) * (len(extent) - dim - 1))

    level = one(*pieces[0])
    for cut in pieces[1:]:
        level = level * one(*cut)
    return level


def shared_out(rng, own, number, rows, number_of, top, reach, skew):
    sequence = jax.random.permutation(rng, number_of)
    packed, ordinary = portions_of(number_of, rows * top, reach, skew, True), portions_of(number_of, rows * top, reach, skew, False)
    places = jnp.arange(number_of)

    def named(tallies, rotation):
        used = int((tallies > 0).sum())
        fixed = max(1, used // 4)
        passed = fixed + (places - fixed + rotation * (used - fixed)) % max(1, number_of - fixed)
        return jnp.zeros((number_of,), jnp.int32).at[sequence[jnp.where(places < fixed, places, passed)]].set(jnp.asarray(tallies, jnp.int32))

    tallies = jnp.where(number % 4 == 0, named(packed, number // 4), named(ordinary, number - number // 4 - 1))
    mixed = jax.random.permutation(jax.random.fold_in(own, 3), number_of)
    donor, sink = mixed[0:number_of // 2 * 2:2], mixed[1:number_of // 2 * 2:2]
    margin = jnp.minimum(tallies[donor] - 1, reach - tallies[sink]) // 2
    margin = jnp.where((donor == sequence[0]) | (sink == sequence[0]) | (tallies[sink] == 0), 0, jnp.maximum(margin, 0))
    passed = jax.random.randint(jax.random.fold_in(own, 4), (number_of // 2,), 0, 1 << 20) % (margin + 1)
    tallies = tallies.at[donor].add(-passed).at[sink].add(passed)
    items = jnp.searchsorted(jnp.cumsum(tallies), jnp.arange(rows * top), side="right").astype(jnp.int32)
    listing = items.reshape(top, rows).T
    listing = listing[jax.random.permutation(jax.random.fold_in(own, 1), rows)]
    rotation = jax.random.randint(jax.random.fold_in(own, 2), (rows, 1), 0, top)
    return jnp.take_along_axis(listing, (jnp.arange(top)[None, :] + rotation) % top, axis=1)


def portions_of(amount, total, most, slope, full):
    weights = [(1 << 20) // math.isqrt(grade ** slope) + 1 for grade in range(1, amount + 1)]
    largest = most if full else min(most, max(-(-total // amount), total * weights[0] // sum(weights)))
    least = 1 if total - largest >= amount - 1 else 0
    counts, spare = [largest] + [least] * (amount - 1), total - largest - least * (amount - 1)
    while spare > 0:
        movable = [i for i in range(1, amount) if counts[i] < largest] or [i for i in range(1, amount) if counts[i] < most]
        mass, budget = sum([weights[i] for i in movable]), spare
        for i in movable:
            addition = min(most - counts[i], max(1, budget * weights[i] // mass), spare)
            counts[i] = counts[i] + addition
            spare = spare - addition
    return np.array(counts)


def gaussian(own_key, dims, deviation, bound, pieces=(), kind=jnp.bfloat16):
    array = jax.random.normal(own_key, dims, jnp.float32) * deviation
    if len(pieces) > 0:
        array = block_levels(own_key, dims, pieces, -0.22, 0.18) * array
    return jnp.clip(array, min=-bound, max=bound).astype(kind)


def setup_inputs(seed: int = 0) -> dict:
    streams_of = jax.random.split(jax.random.key(seed), 14)
    queries = draw_queries(jax.random.fold_in(streams_of[13], 71), 0)
    key_rows = draw_key_rows(jax.random.fold_in(streams_of[13], 71), 0)
    values = gaussian(streams_of[2], (SEQS, LENGTH, KV_HEADS, HEAD_DIM), 1.0, 6.0, ((0, 8), (1, 16)))
    query_gain = draw_query_gain(jax.random.fold_in(streams_of[13], 71), 0)
    key_gain = draw_key_gain(jax.random.fold_in(streams_of[13], 71), 0)
    out_weight = gaussian(streams_of[5], (HEADS * HEAD_DIM, D), (HEADS * HEAD_DIM) ** -0.5, 0.125, ((0, 16), (1, 8)))
    residual = gaussian(streams_of[6], (SEQS, LENGTH, D), 1.0, 6.0, ((0, 8), (1, 16)))
    norm_gain = jnp.clip(1.0 + 0.18 * jax.random.normal(streams_of[7], (D,), jnp.float32), 0.1, 1.9)
    expert_gate = gaussian(streams_of[8], (EXPERTS, D, EXPERT_FF), D ** -0.5, 0.125, ((0, 16),))
    expert_up = gaussian(streams_of[9], (EXPERTS, D, EXPERT_FF), D ** -0.5, 0.125, ((0, 16),))
    expert_down = gaussian(streams_of[10], (EXPERTS, EXPERT_FF, D), EXPERT_FF ** -0.5, 0.125, ((0, 16),))
    routes_keys = jax.random.split(jax.random.fold_in(streams_of[11], 1), SEQS * LENGTH // HALF)
    routes_turns = jax.random.permutation(jax.random.fold_in(streams_of[11], 3), SEQS * LENGTH // HALF)
    routes = jax.vmap(lambda own, number: shared_out(jax.random.fold_in(streams_of[11], 2), own, number, HALF, EXPERTS, 2, CAP, 2))(routes_keys, routes_turns).reshape((SEQS, LENGTH, 2))
    route_weight = jnp.clip(0.25 + 0.75 * jax.random.uniform(streams_of[12], (SEQS, LENGTH, 2), jnp.float32) ** block_levels(streams_of[12], (SEQS, LENGTH, 2), ((0, 8), (1, 16)), -0.2, 0.2), 0.25, 1.0)
    return {"queries": queries, "key_rows": key_rows, "values": values, "query_gain": query_gain, "key_gain": key_gain, "out_weight": out_weight, "residual": residual, "norm_gain": norm_gain, "expert_gate": expert_gate, "expert_up": expert_up, "expert_down": expert_down, "routes": routes, "route_weight": route_weight}


EPS = 1e-06
THETA = 10000.0

def rotate_half(vector, position):
    half_size = vector.shape[-1] // 2
    inverse = THETA ** (-jnp.arange(half_size, dtype=jnp.float32) / half_size)
    angles = position[:, None] * inverse[None, :]
    cosine = jnp.cos(angles)[:, None, :]
    sine_part = jnp.sin(angles)[:, None, :]
    first_part = vector[..., :half_size]
    second_part = vector[..., half_size:]
    return jnp.concatenate([first_part * cosine - second_part * sine_part, first_part * sine_part + second_part * cosine], axis=-1)

def normalize_rotate(vector, gain, positions):
    as_float = vector.astype(jnp.float32)
    scaled = as_float * lax.rsqrt(lax.optimization_barrier(jnp.mean(as_float * as_float, axis=-1, keepdims=True)) + EPS) * gain
    grid_row = (positions // GRID_W).astype(jnp.float32)
    column = (positions % GRID_W).astype(jnp.float32)
    quarter = scaled.shape[-1] // 2
    turned = jnp.concatenate([rotate_half(scaled[..., :quarter], grid_row), rotate_half(scaled[..., quarter:], column)], axis=-1)
    return turned.astype(jnp.bfloat16)

def softmax_rows(scores):
    row_max = lax.optimization_barrier(jnp.max(scores, axis=-1, keepdims=True))
    exponent = jnp.exp(scores - row_max)
    return (exponent / lax.optimization_barrier(jnp.sum(exponent, axis=-1, keepdims=True))).astype(jnp.bfloat16)

def attend_sequence(rot_query, rot_key, value_rows):
    length = rot_query.shape[0]
    group_size = HEADS // KV_HEADS
    block_size = min(512, length)
    key_float = rot_key.astype(jnp.float32)
    value_float = value_rows.astype(jnp.float32)
    grouped = rot_query.reshape(length // block_size, block_size, KV_HEADS, group_size, HEAD_DIM)

    def one_block(query_block):
        scores = jnp.einsum('qhgd,khd->hgqk', query_block.astype(jnp.float32), key_float) * HEAD_DIM ** (-0.5)
        weights = softmax_rows(scores)
        return jnp.einsum('hgqk,khd->qhgd', weights.astype(jnp.float32), value_float).astype(jnp.bfloat16)
    outputs = lax.map(one_block, grouped)
    return outputs.reshape(length, HEADS * HEAD_DIM)

def reference(queries, key_rows, values, query_gain, key_gain, out_weight, residual, norm_gain, expert_gate, expert_up, expert_down, routes, route_weight):
    positions = jnp.arange(LENGTH, dtype=jnp.int32)

    def one_sequence(inputs):
        query_seq, key_seq, value_seq, residual_seq = inputs
        rot_query = normalize_rotate(query_seq, query_gain, positions)
        rot_key = normalize_rotate(key_seq, key_gain, positions)
        attended = attend_sequence(rot_query, rot_key, value_seq)
        return residual_seq.astype(jnp.float32) + jnp.dot(attended, out_weight, preferred_element_type=jnp.float32)
    mixed_sum = lax.map(one_sequence, (queries, key_rows, values, residual))
    flat_mixed = mixed_sum.reshape(-1, D)
    normed = (flat_mixed * lax.rsqrt(lax.optimization_barrier(jnp.mean(flat_mixed * flat_mixed, axis=-1, keepdims=True)) + EPS) * norm_gain).astype(jnp.bfloat16)
    tokens = flat_mixed.shape[0]
    blocks = tokens // HALF
    chosen = routes.reshape(blocks, HALF * 2)
    onehot = (chosen[..., None] == jnp.arange(EXPERTS, dtype=jnp.int32)).astype(jnp.int32)
    slot_rank = lax.optimization_barrier(jnp.sum(jnp.cumsum(onehot, axis=1) * onehot, axis=-1)) - 1
    slot_index = jnp.arange(blocks, dtype=jnp.int32)[:, None] * CAP + slot_rank
    per_expert = blocks * CAP
    target = (chosen * per_expert + slot_index).reshape(-1).astype(jnp.int32)
    source_row = jnp.repeat(jnp.arange(tokens, dtype=jnp.int32), 2)
    row_table = jnp.full((EXPERTS * per_expert,), tokens, jnp.int32).at[target].set(source_row)
    padded = jnp.concatenate([normed, jnp.zeros((1, D), jnp.bfloat16)], axis=0)

    def one_expert(inputs):
        row_ids, gate_weight, up_weight, down_weight = inputs
        selected = padded[row_ids]
        gate_part = jnp.dot(selected, gate_weight, preferred_element_type=jnp.float32)
        up_part = jnp.dot(selected, up_weight, preferred_element_type=jnp.float32)
        hidden = (jax.nn.silu(gate_part) * up_part).astype(jnp.bfloat16)
        return jnp.dot(hidden, down_weight, preferred_element_type=jnp.float32).astype(jnp.bfloat16)
    outputs = lax.map(one_expert, (row_table.reshape(EXPERTS, per_expert), expert_gate, expert_up, expert_down))
    picked = outputs.reshape(-1, D)[target].astype(jnp.float32).reshape(tokens, 2, D)
    weights = route_weight.reshape(tokens, 2, 1)
    result = flat_mixed + lax.optimization_barrier(jnp.sum(picked * weights, axis=1))
    return result.reshape(SEQS, LENGTH, D).astype(jnp.bfloat16)
```

```python
import jax
import jax.numpy as jnp
from jax import lax
from jax.experimental import pallas as pl
from jax.experimental.pallas import tpu as pltpu
from jax.sharding import PartitionSpec as P

MESH = pl.DeviceIdType.MESH

GRID_W = 64


EPS = 1e-06
THETA = 10000.0


def rotate_half(vector, position):
    half_size = vector.shape[-1] // 2
    inverse = THETA ** (-jnp.arange(half_size, dtype=jnp.float32) / half_size)
    angles = position[:, None] * inverse[None, :]
    cosine = jnp.cos(angles)[:, None, :]
    sine_part = jnp.sin(angles)[:, None, :]
    first_part = vector[..., :half_size]
    second_part = vector[..., half_size:]
    return jnp.concatenate(
        [
            first_part * cosine - second_part * sine_part,
            first_part * sine_part + second_part * cosine,
        ],
        axis=-1,
    )


def normalize_rotate(vector, gain, positions):
    as_float = vector.astype(jnp.float32)
    scaled = (
        as_float * lax.rsqrt(jnp.mean(as_float * as_float, axis=-1, keepdims=True) + EPS) * gain
    )
    grid_row = (positions // GRID_W).astype(jnp.float32)
    column = (positions % GRID_W).astype(jnp.float32)
    quarter = scaled.shape[-1] // 2
    turned = jnp.concatenate(
        [rotate_half(scaled[..., :quarter], grid_row), rotate_half(scaled[..., quarter:], column)],
        axis=-1,
    )
    return turned.astype(jnp.bfloat16)


def softmax_rows(scores):
    row_max = jnp.max(scores, axis=-1, keepdims=True)
    exponent = jnp.exp(scores - row_max)
    return (exponent / jnp.sum(exponent, axis=-1, keepdims=True)).astype(jnp.bfloat16)


def attend_block(query_rows, key_rows, value_rows):
    scores = jnp.einsum(
        "qd,kd->qk", query_rows, key_rows, preferred_element_type=jnp.float32
    ) * query_rows.shape[-1] ** (-0.5)
    weights = softmax_rows(scores)
    return jnp.dot(weights, value_rows, preferred_element_type=jnp.float32).astype(jnp.bfloat16)


def attend_heads(head_query, head_key, head_value):
    length, head_count, head_width = head_query.shape
    block_size = min(512, length)
    key_slice = head_key[:, 0]
    value_slice = head_value[:, 0]
    query_blocks = head_query[:, 0].reshape(length // block_size, block_size, head_width)

    def one_block(query_block):
        return attend_block(query_block, key_slice, value_slice)

    outputs = [lax.map(one_block, query_blocks).reshape(length, head_width)]
    return jnp.stack(outputs, axis=1)


def gather_columns(out_weight):
    return lax.all_gather(out_weight, "dp", axis=1, tiled=True)


def project_tokens(attended, out_weight):
    out_cols = gather_columns(out_weight)
    return jnp.dot(
        attended,
        lax.all_gather(out_cols, "sp", axis=0, tiled=True),
        preferred_element_type=jnp.float32,
    )


def on_device(
    queries,
    key_rows,
    values,
    query_gain,
    key_gain,
    out_weight,
    residual,
    norm_gain,
    expert_gate,
    expert_up,
    expert_down,
    routes,
    route_weight,
):
    tok_count = queries.shape[1]
    head_count = queries.shape[2]
    head_width = queries.shape[3]
    group_size = head_count // key_rows.shape[2]
    positions = lax.axis_index("sp") * tok_count + jnp.arange(tok_count, dtype=jnp.int32)
    rot_query = normalize_rotate(queries[0], query_gain, positions)
    rot_key = normalize_rotate(key_rows[0], key_gain, positions)
    value_rows = values[0]
    head_query, head_key, head_value = (
        lax.all_to_all(rot_query, "sp", split_axis=1, concat_axis=0, tiled=True),
        lax.all_to_all(
            jnp.repeat(rot_key, group_size, axis=1), "sp", split_axis=1, concat_axis=0, tiled=True
        ),
        lax.all_to_all(
            jnp.repeat(value_rows, group_size, axis=1),
            "sp",
            split_axis=1,
            concat_axis=0,
            tiled=True,
        ),
    )
    by_heads = attend_heads(head_query, head_key, head_value)
    returned_heads = lax.all_to_all(by_heads, "sp", split_axis=0, concat_axis=1, tiled=True)
    projected = project_tokens(
        returned_heads.reshape(tok_count, head_count * head_width), out_weight
    )
    mixed_sum = residual[0].astype(jnp.float32) + projected
    return moe(
        mixed_sum, norm_gain, routes[0], route_weight[0], expert_gate[0], expert_up[0], expert_down[0]
    )[None]


def offset_of(i):
    q = i // 4
    return (q % 2) * 2 + q // 2, i % 4


def peer_of(z, x, dz, dx):
    return ((z + dz) % 4) * 4 + (x + dx) % 4


def experts_of_slots(slots, z, x):
    i = slots >> 5
    q = i >> 2
    dz = ((q & 1) << 1) | (q >> 1)
    return (((z + dz) & 3) << 2) | ((x + (i & 3)) & 3)


def to_bf16(mask):
    return jnp.where(mask, 1.0, 0.0).astype(jnp.bfloat16)


def moe_kernel(
    mixed_ref, gain_ref, routes_ref, routes_t_ref, weight_ref, gate_hbm, up_hbm, down_hbm,
    out_ref,
    gate_v, up_v, down_v, send_v, recv_v, res_v, ret_v, hid_v,
    w_sem, ds_sem, dr_sem, rs_sem, rr_sem,
):
    me = lax.axis_index("sp")
    z, x = me // 4, me % 4
    loads = [
        pltpu.make_async_copy(src, dst, w_sem.at[n])
        for n, (src, dst) in enumerate(((gate_hbm, gate_v), (up_hbm, up_v), (down_hbm, down_v)))
    ]
    for load in loads:
        load.start()
    barrier = pltpu.get_barrier_semaphore()
    for i in range(1, 16):
        dz, dx = offset_of(i)
        pl.semaphore_signal(
            barrier, inc=1, device_id={"sp": peer_of(z, x, dz, dx)}, device_id_type=MESH
        )

    mixed = mixed_ref[...]
    scale = lax.rsqrt(jnp.mean(mixed * mixed, axis=-1, keepdims=True) + EPS)
    normed = (mixed * scale * gain_ref[...]).astype(jnp.bfloat16)

    slots = lax.broadcasted_iota(jnp.int32, (512, 128), 0)
    rows = lax.broadcasted_iota(jnp.int32, (512, 128), 1)
    expert = experts_of_slots(slots, z, x)
    named = (routes_t_ref[0:1, :] == expert) | (routes_t_ref[1:2, :] == expert)
    before_r = lax.broadcasted_iota(jnp.int32, (128, 128), 0)
    before_c = lax.broadcasted_iota(jnp.int32, (128, 128), 1)
    same = (before_r >> 6) == (before_c >> 6)
    upper = to_bf16((before_r < before_c) & same)
    lower = to_bf16((before_c < before_r) & same)
    rank = jnp.dot(to_bf16(named), upper, preferred_element_type=jnp.float32)
    wanted = ((slots & 31) - ((rows >> 6) << 4)).astype(jnp.float32)
    pick = to_bf16(named & (rank == wanted))
    for c in range(2):
        part = slice(c * 256, c * 256 + 256)
        for n in range(4):
            cols = slice(n * 512, n * 512 + 512)
            sent = jnp.dot(
                pick[part], normed[:, cols], preferred_element_type=jnp.float32
            ).astype(jnp.bfloat16)
            send_v[part, cols] = sent
            if c == 0:
                recv_v[0:32, cols] = sent[0:32]
    pl.semaphore_wait(barrier, 15)

    def copy(i, src, dst, ssem, rsem, dz, dx):
        return pltpu.make_async_remote_copy(
            src_ref=src.at[pl.ds(i * 32, 32)],
            dst_ref=dst.at[pl.ds(i * 32, 32)],
            send_sem=ssem.at[i],
            recv_sem=rsem.at[i],
            device_id={"sp": peer_of(z, x, dz, dx)},
            device_id_type=MESH,
        )

    outgoing = []
    for i in range(1, 16):
        dz, dx = offset_of(i)
        outgoing.append(copy(i, send_v, recv_v, ds_sem, dr_sem, dz, dx))
    for sending in outgoing:
        sending.start()

    slots_t = lax.broadcasted_iota(jnp.int32, (128, 512), 1)
    rows_t = lax.broadcasted_iota(jnp.int32, (128, 512), 0)
    expert_t = experts_of_slots(slots_t, z, x)
    first = routes_ref[:, 0:1] == expert_t
    second = routes_ref[:, 1:2] == expert_t
    rank_t = jnp.dot(lower, to_bf16(first | second), preferred_element_type=jnp.float32)
    here = rank_t == ((slots_t & 31) - ((rows_t >> 6) << 4)).astype(jnp.float32)
    take_first = to_bf16(first & here)
    take_second = to_bf16(second & here)

    returning = []
    for i in range(1, 16):
        dz, dx = offset_of(i)
        returning.append(copy(i, res_v, ret_v, rs_sem, rr_sem, -dz, -dx))
    loads[0].wait()
    loads[1].wait()
    for c in range(2):
        for i in range(max(1, c * 8), c * 8 + 8):
            outgoing[i - 1].wait_recv()
        part = slice(c * 256, c * 256 + 256)
        for n in range(7):
            cols = slice(n * 256, n * 256 + 256)
            gate = jnp.dot(recv_v[part], gate_v[:, cols], preferred_element_type=jnp.float32)
            up = jnp.dot(recv_v[part], up_v[:, cols], preferred_element_type=jnp.float32)
            hid_v[:, cols] = (gate / (1.0 + jnp.exp(-gate)) * up).astype(jnp.bfloat16)
        if c == 0:
            loads[2].wait()
        for n in range(8):
            cols = slice(n * 256, n * 256 + 256)
            done = jnp.dot(
                hid_v[...], down_v[:, cols], preferred_element_type=jnp.float32
            ).astype(jnp.bfloat16)
            res_v[part, cols] = done
            if c == 0:
                ret_v[0:32, cols] = done[0:32]
        for i in range(max(1, c * 8), c * 8 + 8):
            returning[i - 1].start()
    for back in returning:
        back.wait_recv()
    for n in range(4):
        cols = slice(n * 512, n * 512 + 512)
        got = ret_v[:, cols]
        one = jnp.dot(take_first, got, preferred_element_type=jnp.float32)
        two = jnp.dot(take_second, got, preferred_element_type=jnp.float32)
        total = mixed_ref[:, cols] + (one * weight_ref[:, 0:1] + two * weight_ref[:, 1:2])
        out_ref[:, cols] = total.astype(jnp.bfloat16)
    for sending in outgoing:
        sending.wait_send()
    for back in returning:
        back.wait_send()


def moe(mixed_sum, norm_gain, routes, route_weight, gate, up, down):
    vmem = pl.BlockSpec(memory_space=pltpu.VMEM)
    hbm = pl.BlockSpec(memory_space=pl.ANY)
    rows = pltpu.VMEM((512, 2048), jnp.bfloat16)
    return pl.pallas_call(
        moe_kernel,
        out_shape=jax.ShapeDtypeStruct((128, 2048), jnp.bfloat16),
        in_specs=[vmem] * 5 + [hbm] * 3,
        out_specs=vmem,
        scratch_shapes=[
            pltpu.VMEM((2048, 1792), jnp.bfloat16),
            pltpu.VMEM((2048, 1792), jnp.bfloat16),
            pltpu.VMEM((1792, 2048), jnp.bfloat16),
            rows, rows, rows, rows,
            pltpu.VMEM((256, 1792), jnp.bfloat16),
            pltpu.SemaphoreType.DMA((3,)),
            pltpu.SemaphoreType.DMA((16,)),
            pltpu.SemaphoreType.DMA((16,)),
            pltpu.SemaphoreType.DMA((16,)),
            pltpu.SemaphoreType.DMA((16,)),
        ],
        compiler_params=pltpu.CompilerParams(
            collective_id=1, has_side_effects=True, vmem_limit_bytes=56 << 20
        ),
        name="experts",
    )(mixed_sum, norm_gain.reshape(1, -1), routes, routes.T, route_weight, gate, up, down)


def solution(mesh):
    in_specs = (
        P("dp", "sp", None, None),
        P("dp", "sp", None, None),
        P("dp", "sp", None, None),
        P(),
        P(),
        P("sp", "dp"),
        P("dp", "sp", None),
        P(),
        P("sp", None, None),
        P("sp", None, None),
        P("sp", None, None),
        P("dp", "sp", None),
        P("dp", "sp", None),
    )
    out_specs = P("dp", "sp", None)
    return jax.shard_map(
        on_device, mesh=mesh, in_specs=in_specs, out_specs=out_specs, check_vma=False
    )
```

```python
import math

import jax
import jax.numpy as jnp
from jax import lax
from jax.experimental import pallas as pl
from jax.experimental.pallas import tpu as pltpu
from jax.sharding import PartitionSpec as P

MESH = pl.DeviceIdType.MESH
EPS = 1e-06
THETA = 10000.0


PIECES = (
    ((0, 64), ("z", "x", "y")),
    ((64, 96), ("y", "x", "z")),
    ((96, 128), ("y", "z", "x")),
)
AXES = ("y", "z", "x")


def front_kernel(
    q_ref, k_ref, v_ref, q_gain_ref, k_gain_ref, residual_hbm, weight_hbm,
    out_ref,
    q_f32, q_send, q_all, kv_send, kv_all, o_send, o_all, att_v, w_all, residual_v,
    local_sem, k1_s, k1_r, k2_s, k2_r, q_s, q_r, o_s, o_r, w_s, w_r, p_s, p_r,
):
    me = lax.axis_index("sp")
    dp = lax.axis_index("dp")
    at = {"z": me // 4, "x": me % 4, "y": dp // 2}
    z, x, y, core = at["z"], at["x"], at["y"], dp % 2

    def device(axis, off):
        if axis == "core":
            return {"dp": y * 2 + (1 - core)}
        v = (at[axis] + off + 4) % 4
        if axis == "y":
            return {"dp": v * 2 + core}
        return {"sp": v * 4 + x if axis == "z" else z * 4 + v}

    def remote(src, dst, ssem, rsem, target):
        return pltpu.make_async_remote_copy(
            src_ref=src, dst_ref=dst, send_sem=ssem, recv_sem=rsem,
            device_id=target, device_id_type=MESH,
        )

    def piece_ref(p, gathered, axis, value, cols=None, owner=None):
        rows = pl.ds(PIECES[p][0][0], PIECES[p][0][1] - PIECES[p][0][0])
        index = [core if owner is None else owner]
        for name in AXES:
            if name == axis:
                index.append(value)
            else:
                index.append(slice(None) if name in gathered else at[name])
        index += [rows, slice(None) if cols is None else cols]
        return w_all.at[tuple(index)]

    load_w = pltpu.make_async_copy(weight_hbm, w_all.at[core, y, z, x], local_sem.at[0])
    load_r = pltpu.make_async_copy(residual_hbm, residual_v, local_sem.at[1])
    load_w.start()
    load_r.start()
    barrier = pltpu.get_barrier_semaphore()
    for axis in AXES:
        for off in (1, 2, 3):
            pl.semaphore_signal(barrier, inc=1, device_id=device(axis, off), device_id_type=MESH)
    pl.semaphore_signal(barrier, inc=1, device_id=device("core", 1), device_id_type=MESH)

    lane = lax.broadcasted_iota(jnp.int32, (128, 128), 1)
    position = lax.broadcasted_iota(jnp.int32, (128, 128), 0) + me * 128
    place = jnp.where(lane < 64, position >> 6, position & 63).astype(jnp.float32)
    rate = jnp.exp((lane & 31).astype(jnp.float32) * (-math.log(THETA) / 32))
    angle = place * rate
    cosine = jnp.cos(angle)
    low = (lane & 63) < 32
    sine = jnp.where(low, -jnp.sin(angle), jnp.sin(angle))

    def turned(rows, gain):
        scaled = rows * lax.rsqrt(jnp.mean(rows * rows, axis=-1, keepdims=True) + EPS) * gain
        other = jnp.where(low, pltpu.roll(scaled, 96, 1), pltpu.roll(scaled, 32, 1))
        return (scaled * cosine + other * sine).astype(jnp.bfloat16)

    for h in range(4):
        part = slice(h * 128, h * 128 + 128)
        kv_send[h, 0] = turned(k_ref[:, part].astype(jnp.float32), k_gain_ref[...])
        kv_send[h, 1] = v_ref[:, part]
    kv_all[x * 4 + z] = kv_send[z]
    q_f32[...] = q_ref[...].reshape(2048, 128).astype(jnp.float32)
    pl.semaphore_wait(barrier, 10)

    def kv_in(off):
        return remote(kv_send.at[(z + off) % 4], kv_all.at[x * 4 + z], k1_s.at[off], k1_r.at[off], device("z", off))

    started = []

    def start(copy):
        copy.start()
        started.append(copy)

    def spread(off):
        slot = kv_all.at[x * 4 + (z - off + 4) % 4]
        for dx in (1, 3, 2):
            start(remote(slot, slot, k2_s.at[off, dx], k2_r.at[off, dx], device("x", dx)))

    for off in (1, 3, 2):
        start(kv_in(off))
    spread(0)

    for h in range(16):
        q_send[h // 4, h % 4] = turned(q_f32[pl.ds(h, 128, stride=16), :], q_gain_ref[...])
    q_all[z] = q_send[z]
    for off in (2, 1, 3):
        start(remote(q_send.at[(z + off) % 4], q_all.at[z], q_s.at[off], q_r.at[off], device("z", off)))

    def phase_copy(p, n, off, outgoing):
        order = PIECES[p][1]
        gathered, axis = order[:n], order[n]
        value = at[axis] if outgoing else (at[axis] - off + 4) % 4
        block = piece_ref(p, gathered, axis, value)
        return remote(block, block, w_s.at[p, n, off], w_r.at[p, n, off], device(axis, off))

    def half_copy(p, side, outgoing):
        order = PIECES[p][1]
        axis = order[2]
        step = 1 if side == 0 else 3
        value = (at[axis] - step + 4) % 4 if outgoing else (at[axis] + 2) % 4
        block = piece_ref(p, order[:2], axis, value, cols=pl.ds(side * 128, 128))
        n = 2 if side == 0 else 0
        return remote(block, block, w_s.at[p, 2, n], w_r.at[p, 2, n], device(axis, step))

    def across(p, part, outgoing):
        order = PIECES[p][1]
        axis = order[2]
        owner = core if outgoing else 1 - core
        cols = None
        if part == 0:
            value = at[axis]
        elif part < 3:
            value = (at[axis] - (1, 3)[part - 1] + 4) % 4
        else:
            value = (at[axis] + 2) % 4
            cols = pl.ds((part - 3) * 128, 128)
        block = piece_ref(p, order[:2], axis, value, cols=cols, owner=owner)
        return remote(block, block, p_s.at[p, part], p_r.at[p, part], device("core", 1))

    load_w.wait()
    for p in range(3):
        for off in (1, 3, 2):
            start(phase_copy(p, 0, off, True))

    for off in (1, 3, 2):
        incoming = kv_all.at[x * 4 + (z - off + 4) % 4]
        remote(incoming, incoming, k1_s.at[off], k1_r.at[off], device("z", off)).wait_recv()
        spread(off)

    for p in range(3):
        for off in (1, 3, 2):
            phase_copy(p, 0, off, False).wait_recv()
        for off in (1, 3, 2):
            start(phase_copy(p, 1, off, True))

    for off in range(4):
        for dx in (1, 3, 2):
            slot = kv_all.at[((x - dx + 4) % 4) * 4 + (z - off + 4) % 4]
            remote(slot, slot, k2_s.at[off, dx], k2_r.at[off, dx], device("x", dx)).wait_recv()

    for p in range(3):
        for off in (1, 3, 2):
            phase_copy(p, 1, off, False).wait_recv()
        for off in (1, 3):
            start(phase_copy(p, 2, off, True))
        start(across(p, 0, True))

    keys = kv_all[:, 0].reshape(2048, 128)
    vals = kv_all[:, 1].reshape(2048, 128)
    factor = 128 ** -0.5 * math.log2(math.e)

    def attend(source, target):
        for half in range(2):
            query = q_all[source, pl.ds(half * 2, 2)].reshape(256, 128)
            scores = lax.dot_general(
                query, keys, (((1,), (1,)), ((), ())), preferred_element_type=jnp.float32
            )
            top = jnp.max(scores, axis=-1, keepdims=True)
            power = jnp.exp2((scores - top) * factor)
            share = (power * (1.0 / jnp.sum(power, axis=-1, keepdims=True))).astype(jnp.bfloat16)
            mixed = jnp.dot(share, vals, preferred_element_type=jnp.float32).astype(jnp.bfloat16)
            target[pl.ds(half * 2, 2)] = mixed.reshape(2, 128, 128)

    for off in (2, 1, 3):
        source = (z - off + 4) % 4
        slot = q_all.at[source]
        remote(slot, slot, q_s.at[off], q_r.at[off], device("z", off)).wait_recv()
        attend(source, o_send.at[source])
        start(remote(o_send.at[source], o_all.at[z], o_s.at[off], o_r.at[off], device("z", -off)))
    attend(z, o_all.at[z])

    for p in (1, 2, 0):
        for side, off in ((0, 1), (1, 3)):
            phase_copy(p, 2, off, False).wait_recv()
            start(half_copy(p, side, True))
            start(across(p, 1 + side, True))
    for p in (1, 2, 0):
        for side in (0, 1):
            half_copy(p, side, False).wait_recv()
            start(across(p, 3 + side, True))
    for off in (2, 1, 3):
        slot = o_all.at[(z + off) % 4]
        remote(slot, slot, o_s.at[off], o_r.at[off], device("z", off)).wait_recv()
    for h in range(16):
        att_v[:, h * 128:h * 128 + 128] = o_all[h // 4, h % 4]
    for p in range(3):
        for part in range(5):
            across(p, part, False).wait_recv()
    load_r.wait()
    for c in range(2):
        for b in range(4):
            first = (b * 2 + c) * 256
            cols = slice(first, first + 256)
            summed = jnp.dot(
                att_v[...], w_all[c, b].reshape(2048, 256), preferred_element_type=jnp.float32
            )
            out_ref[:, cols] = residual_v[:, cols].astype(jnp.float32) + summed
    for copy in started:
        copy.wait_send()


def front(queries, key_rows, values, query_gain, key_gain, residual, out_weight):
    vmem = pl.BlockSpec(memory_space=pltpu.VMEM)
    hbm = pl.BlockSpec(memory_space=pl.ANY)
    dma = pltpu.SemaphoreType.DMA
    heads = pltpu.VMEM((4, 4, 128, 128), jnp.bfloat16)
    return pl.pallas_call(
        front_kernel,
        out_shape=jax.ShapeDtypeStruct((128, 2048), jnp.float32),
        in_specs=[vmem] * 5 + [hbm] * 2,
        out_specs=vmem,
        scratch_shapes=[
            pltpu.VMEM((2048, 128), jnp.float32),
            heads, heads,
            pltpu.VMEM((4, 2, 128, 128), jnp.bfloat16),
            pltpu.VMEM((16, 2, 128, 128), jnp.bfloat16),
            heads, heads,
            pltpu.VMEM((128, 2048), jnp.bfloat16),
            pltpu.VMEM((2, 4, 4, 4, 128, 256), jnp.bfloat16),
            pltpu.VMEM((128, 2048), jnp.bfloat16),
            dma((2,)),
            dma((4,)), dma((4,)), dma((4, 4)), dma((4, 4)),
            dma((4,)), dma((4,)), dma((4,)), dma((4,)),
            dma((3, 3, 4)), dma((3, 3, 4)), dma((3, 5)), dma((3, 5)),
        ],
        compiler_params=pltpu.CompilerParams(
            collective_id=0, has_side_effects=True, vmem_limit_bytes=48 << 20
        ),
        name="front",
    )(
        queries, key_rows.reshape(128, 512), values.reshape(128, 512),
        query_gain.reshape(1, 128), key_gain.reshape(1, 128), residual, out_weight,
    )


def offset_of(i):
    q = i // 4
    return (q % 2) * 2 + q // 2, i % 4


def peer_of(z, x, dz, dx):
    return ((z + dz) % 4) * 4 + (x + dx) % 4


def experts_of_slots(slots, z, x):
    i = slots >> 5
    q = i >> 2
    dz = ((q & 1) << 1) | (q >> 1)
    return (((z + dz) & 3) << 2) | ((x + (i & 3)) & 3)


def to_bf16(mask):
    return jnp.where(mask, 1.0, 0.0).astype(jnp.bfloat16)


def moe_kernel(
    mixed_ref, gain_ref, routes_ref, routes_t_ref, weight_ref, gate_hbm, up_hbm, down_hbm,
    out_ref,
    gate_v, up_v, down_v, send_v, recv_v, res_v, ret_v, hid_v,
    w_sem, ds_sem, dr_sem, rs_sem, rr_sem,
):
    me = lax.axis_index("sp")
    z, x = me // 4, me % 4
    loads = [
        pltpu.make_async_copy(src, dst, w_sem.at[n])
        for n, (src, dst) in enumerate(((gate_hbm, gate_v), (up_hbm, up_v), (down_hbm, down_v)))
    ]
    for load in loads:
        load.start()
    barrier = pltpu.get_barrier_semaphore()
    for i in range(1, 16):
        dz, dx = offset_of(i)
        pl.semaphore_signal(
            barrier, inc=1, device_id={"sp": peer_of(z, x, dz, dx)}, device_id_type=MESH
        )

    mixed = mixed_ref[...]
    scale = lax.rsqrt(jnp.mean(mixed * mixed, axis=-1, keepdims=True) + EPS)
    normed = (mixed * scale * gain_ref[...]).astype(jnp.bfloat16)

    slots = lax.broadcasted_iota(jnp.int32, (512, 128), 0)
    rows = lax.broadcasted_iota(jnp.int32, (512, 128), 1)
    expert = experts_of_slots(slots, z, x)
    named = (routes_t_ref[0:1, :] == expert) | (routes_t_ref[1:2, :] == expert)
    before_r = lax.broadcasted_iota(jnp.int32, (128, 128), 0)
    before_c = lax.broadcasted_iota(jnp.int32, (128, 128), 1)
    same = (before_r >> 6) == (before_c >> 6)
    upper = to_bf16((before_r < before_c) & same)
    lower = to_bf16((before_c < before_r) & same)
    rank = jnp.dot(to_bf16(named), upper, preferred_element_type=jnp.float32)
    wanted = ((slots & 31) - ((rows >> 6) << 4)).astype(jnp.float32)
    pick = to_bf16(named & (rank == wanted))
    for c in range(2):
        part = slice(c * 256, c * 256 + 256)
        for n in range(4):
            cols = slice(n * 512, n * 512 + 512)
            sent = jnp.dot(
                pick[part], normed[:, cols], preferred_element_type=jnp.float32
            ).astype(jnp.bfloat16)
            send_v[part, cols] = sent
            if c == 0:
                recv_v[0:32, cols] = sent[0:32]
    pl.semaphore_wait(barrier, 15)

    def copy(i, src, dst, ssem, rsem, dz, dx):
        return pltpu.make_async_remote_copy(
            src_ref=src.at[pl.ds(i * 32, 32)],
            dst_ref=dst.at[pl.ds(i * 32, 32)],
            send_sem=ssem.at[i],
            recv_sem=rsem.at[i],
            device_id={"sp": peer_of(z, x, dz, dx)},
            device_id_type=MESH,
        )

    outgoing = []
    for i in range(1, 16):
        dz, dx = offset_of(i)
        outgoing.append(copy(i, send_v, recv_v, ds_sem, dr_sem, dz, dx))
    for sending in outgoing:
        sending.start()

    slots_t = lax.broadcasted_iota(jnp.int32, (128, 512), 1)
    rows_t = lax.broadcasted_iota(jnp.int32, (128, 512), 0)
    expert_t = experts_of_slots(slots_t, z, x)
    first = routes_ref[:, 0:1] == expert_t
    second = routes_ref[:, 1:2] == expert_t
    rank_t = jnp.dot(lower, to_bf16(first | second), preferred_element_type=jnp.float32)
    here = rank_t == ((slots_t & 31) - ((rows_t >> 6) << 4)).astype(jnp.float32)
    take_first = to_bf16(first & here)
    take_second = to_bf16(second & here)

    returning = []
    for i in range(1, 16):
        dz, dx = offset_of(i)
        returning.append(copy(i, res_v, ret_v, rs_sem, rr_sem, -dz, -dx))
    loads[0].wait()
    loads[1].wait()
    for c in range(2):
        for i in range(max(1, c * 8), c * 8 + 8):
            outgoing[i - 1].wait_recv()
        part = slice(c * 256, c * 256 + 256)
        for n in range(7):
            cols = slice(n * 256, n * 256 + 256)
            gate = jnp.dot(recv_v[part], gate_v[:, cols], preferred_element_type=jnp.float32)
            up = jnp.dot(recv_v[part], up_v[:, cols], preferred_element_type=jnp.float32)
            hid_v[:, cols] = (gate / (1.0 + jnp.exp(-gate)) * up).astype(jnp.bfloat16)
        if c == 0:
            loads[2].wait()
        for n in range(8):
            cols = slice(n * 256, n * 256 + 256)
            done = jnp.dot(
                hid_v[...], down_v[:, cols], preferred_element_type=jnp.float32
            ).astype(jnp.bfloat16)
            res_v[part, cols] = done
            if c == 0:
                ret_v[0:32, cols] = done[0:32]
        for i in range(max(1, c * 8), c * 8 + 8):
            returning[i - 1].start()
    for back in returning:
        back.wait_recv()
    for n in range(4):
        cols = slice(n * 512, n * 512 + 512)
        got = ret_v[:, cols]
        one = jnp.dot(take_first, got, preferred_element_type=jnp.float32)
        two = jnp.dot(take_second, got, preferred_element_type=jnp.float32)
        total = mixed_ref[:, cols] + (one * weight_ref[:, 0:1] + two * weight_ref[:, 1:2])
        out_ref[:, cols] = total.astype(jnp.bfloat16)
    for sending in outgoing:
        sending.wait_send()
    for back in returning:
        back.wait_send()


def moe(mixed_sum, norm_gain, routes, route_weight, gate, up, down):
    vmem = pl.BlockSpec(memory_space=pltpu.VMEM)
    hbm = pl.BlockSpec(memory_space=pl.ANY)
    rows = pltpu.VMEM((512, 2048), jnp.bfloat16)
    return pl.pallas_call(
        moe_kernel,
        out_shape=jax.ShapeDtypeStruct((128, 2048), jnp.bfloat16),
        in_specs=[vmem] * 5 + [hbm] * 3,
        out_specs=vmem,
        scratch_shapes=[
            pltpu.VMEM((2048, 1792), jnp.bfloat16),
            pltpu.VMEM((2048, 1792), jnp.bfloat16),
            pltpu.VMEM((1792, 2048), jnp.bfloat16),
            rows, rows, rows, rows,
            pltpu.VMEM((256, 1792), jnp.bfloat16),
            pltpu.SemaphoreType.DMA((3,)),
            pltpu.SemaphoreType.DMA((16,)),
            pltpu.SemaphoreType.DMA((16,)),
            pltpu.SemaphoreType.DMA((16,)),
            pltpu.SemaphoreType.DMA((16,)),
        ],
        compiler_params=pltpu.CompilerParams(
            collective_id=1, has_side_effects=True, vmem_limit_bytes=56 << 20
        ),
        name="experts",
    )(mixed_sum, norm_gain.reshape(1, -1), routes, routes.T, route_weight, gate, up, down)


def on_device(
    queries,
    key_rows,
    values,
    query_gain,
    key_gain,
    out_weight,
    residual,
    norm_gain,
    expert_gate,
    expert_up,
    expert_down,
    routes,
    route_weight,
):
    mixed_sum = front(
        queries[0], key_rows[0], values[0], query_gain, key_gain, residual[0], out_weight
    )
    return moe(
        mixed_sum, norm_gain, routes[0], route_weight[0], expert_gate[0], expert_up[0], expert_down[0]
    )[None]


def solution(mesh):
    in_specs = (
        P("dp", "sp", None, None),
        P("dp", "sp", None, None),
        P("dp", "sp", None, None),
        P(),
        P(),
        P("sp", "dp"),
        P("dp", "sp", None),
        P(),
        P("sp", None, None),
        P("sp", None, None),
        P("sp", None, None),
        P("dp", "sp", None),
        P("dp", "sp", None),
    )
    out_specs = P("dp", "sp", None)
    return jax.shard_map(
        on_device, mesh=mesh, in_specs=in_specs, out_specs=out_specs, check_vma=False
    )
```

```python
import math

import jax
import jax.numpy as jnp
from jax import lax
from jax.experimental import pallas as pl
from jax.experimental.pallas import tpu as pltpu
from jax.sharding import PartitionSpec as P

MESH = pl.DeviceIdType.MESH
EPS = 1e-06
THETA = 10000.0
PIECES = (
    ((0, 64), ("z", "x", "y")),
    ((64, 96), ("y", "x", "z")),
    ((96, 128), ("y", "z", "x")),
)
AXES = ("y", "z", "x")


def offset_of(i):
    q = i // 4
    return (q % 2) * 2 + q // 2, i % 4


def peer_of(z, x, dz, dx):
    return ((z + dz) % 4) * 4 + (x + dx) % 4


def experts_of_slots(slots, z, x):
    i = slots >> 5
    q = i >> 2
    dz = ((q & 1) << 1) | (q >> 1)
    return (((z + dz) & 3) << 2) | ((x + (i & 3)) & 3)


def to_bf16(mask):
    return jnp.where(mask, 1.0, 0.0).astype(jnp.bfloat16)


def layer_kernel(
    q_hbm, k_hbm, v_hbm, q_gain_hbm, k_gain_hbm, weight_hbm, residual_hbm, norm_gain_hbm,
    gate_hbm, up_hbm, down_hbm, routes_hbm, share_hbm,
    out_hbm,
    q_raw, k_raw, v_raw, q_gain_ref, k_gain_ref, norm_gain_ref, routes_ref, share_ref,
    k_f32, v_f32, q_f32, q_send, q_all, kv_send, kv_all, o_send, o_all, att_v, w_all, residual_v,
    mixed_ref, pick_v, take_v,
    gate_v, up_v, down_v, send_v, recv_v, res_v, ret_v, hid_v, out_v,
    local_sem, k1_s, k1_r, k2_s, k2_r, q_s, q_r, o_s, o_r, w_s, w_r, p_s, p_r,
    ds_sem, dr_sem, rs_sem, rr_sem,
):
    me = lax.axis_index("sp")
    dp = lax.axis_index("dp")
    at = {"z": me // 4, "x": me % 4, "y": dp // 2}
    z, x, y, core = at["z"], at["x"], at["y"], dp % 2

    def device(axis, off):
        if axis == "core":
            return {"dp": y * 2 + (1 - core)}
        v = (at[axis] + off + 4) % 4
        if axis == "y":
            return {"dp": v * 2 + core}
        return {"sp": v * 4 + x if axis == "z" else z * 4 + v}

    def remote(src, dst, ssem, rsem, target):
        return pltpu.make_async_remote_copy(
            src_ref=src, dst_ref=dst, send_sem=ssem, recv_sem=rsem,
            device_id=target, device_id_type=MESH,
        )

    def piece_ref(p, gathered, axis, value, cols=None, owner=None):
        rows = pl.ds(PIECES[p][0][0], PIECES[p][0][1] - PIECES[p][0][0])
        index = [core if owner is None else owner]
        for name in AXES:
            if name == axis:
                index.append(value)
            else:
                index.append(slice(None) if name in gathered else at[name])
        index += [rows, slice(None) if cols is None else cols]
        return w_all.at[tuple(index)]

    barrier = pltpu.get_barrier_semaphore()
    for i in range(1, 16):
        pl.semaphore_signal(
            barrier, inc=1, device_id={"sp": peer_of(z, x, *offset_of(i))}, device_id_type=MESH
        )
    for off in (1, 2, 3):
        pl.semaphore_signal(barrier, inc=1, device_id=device("y", off), device_id_type=MESH)
    pl.semaphore_signal(barrier, inc=1, device_id=device("core", 1), device_id_type=MESH)
    loads = [
        pltpu.make_async_copy(src, dst, local_sem.at[n])
        for n, (src, dst) in enumerate(
            (
                (k_hbm, k_raw), (v_hbm, v_raw), (k_gain_hbm, k_gain_ref), (q_gain_hbm, q_gain_ref),
                (q_hbm, q_raw), (weight_hbm, w_all.at[core, y, z, x]), (residual_hbm, residual_v),
                (norm_gain_hbm, norm_gain_ref), (routes_hbm, routes_ref), (share_hbm, share_ref),
                (gate_hbm, gate_v), (up_hbm, up_v), (down_hbm, down_v),
            )
        )
    ]
    for load in loads:
        load.start()

    lane = lax.broadcasted_iota(jnp.int32, (128, 128), 1)
    position = lax.broadcasted_iota(jnp.int32, (128, 128), 0) + me * 128
    place = jnp.where(lane < 64, position >> 6, position & 63).astype(jnp.float32)
    rate = jnp.exp((lane & 31).astype(jnp.float32) * (-math.log(THETA) / 32))
    angle = place * rate
    cosine = jnp.cos(angle)
    low = (lane & 63) < 32
    sine = jnp.where(low, -jnp.sin(angle), jnp.sin(angle))

    def turned(rows, gain):
        scaled = rows * lax.rsqrt(jnp.mean(rows * rows, axis=-1, keepdims=True) + EPS) * gain
        other = jnp.where(low, pltpu.roll(scaled, 96, 1), pltpu.roll(scaled, 32, 1))
        return (scaled * cosine + other * sine).astype(jnp.bfloat16)

    for load in loads[:4]:
        load.wait()
    k_f32[...] = k_raw[...].astype(jnp.float32)
    v_f32[...] = v_raw[...].astype(jnp.float32)
    for h in range(4):
        kv_send[h, 0] = turned(k_f32[:, h, :], k_gain_ref[...])
        kv_send[h, 1] = v_f32[:, h, :].astype(jnp.bfloat16)
    kv_all[x * 4 + z] = kv_send[z]
    loads[4].wait()
    q_f32[...] = q_raw[...].reshape(2048, 128).astype(jnp.float32)
    pl.semaphore_wait(barrier, 19)

    def kv_in(off):
        return remote(kv_send.at[(z + off) % 4], kv_all.at[x * 4 + z], k1_s.at[off], k1_r.at[off], device("z", off))

    started = []

    def start(copy):
        copy.start()
        started.append(copy)

    def spread(off):
        slot = kv_all.at[x * 4 + (z - off + 4) % 4]
        for dx in (1, 3, 2):
            start(remote(slot, slot, k2_s.at[off, dx], k2_r.at[off, dx], device("x", dx)))

    for off in (1, 3, 2):
        start(kv_in(off))
    spread(0)

    for h in range(16):
        q_send[h // 4, h % 4] = turned(q_f32[pl.ds(h, 128, stride=16), :], q_gain_ref[...])
    q_all[z] = q_send[z]
    for off in (2, 1, 3):
        start(remote(q_send.at[(z + off) % 4], q_all.at[z], q_s.at[off], q_r.at[off], device("z", off)))

    def phase_copy(p, n, off, outgoing):
        order = PIECES[p][1]
        gathered, axis = order[:n], order[n]
        value = at[axis] if outgoing else (at[axis] - off + 4) % 4
        block = piece_ref(p, gathered, axis, value)
        return remote(block, block, w_s.at[p, n, off], w_r.at[p, n, off], device(axis, off))

    def half_copy(p, side, outgoing):
        order = PIECES[p][1]
        axis = order[2]
        step = 1 if side == 0 else 3
        value = (at[axis] - step + 4) % 4 if outgoing else (at[axis] + 2) % 4
        block = piece_ref(p, order[:2], axis, value, cols=pl.ds(side * 128, 128))
        n = 2 if side == 0 else 0
        return remote(block, block, w_s.at[p, 2, n], w_r.at[p, 2, n], device(axis, step))

    def across(p, part, outgoing):
        order = PIECES[p][1]
        axis = order[2]
        owner = core if outgoing else 1 - core
        cols = None
        if part == 0:
            value = at[axis]
        elif part < 3:
            value = (at[axis] - (1, 3)[part - 1] + 4) % 4
        else:
            value = (at[axis] + 2) % 4
            cols = pl.ds((part - 3) * 128, 128)
        block = piece_ref(p, order[:2], axis, value, cols=cols, owner=owner)
        return remote(block, block, p_s.at[p, part], p_r.at[p, part], device("core", 1))

    loads[5].wait()
    for p in range(3):
        for off in (1, 3, 2):
            start(phase_copy(p, 0, off, True))

    for off in (1, 3, 2):
        incoming = kv_all.at[x * 4 + (z - off + 4) % 4]
        remote(incoming, incoming, k1_s.at[off], k1_r.at[off], device("z", off)).wait_recv()
        spread(off)

    for p in range(3):
        for off in (1, 3, 2):
            phase_copy(p, 0, off, False).wait_recv()
        for off in (1, 3, 2):
            start(phase_copy(p, 1, off, True))

    for load in loads[7:10]:
        load.wait()
    slots = lax.broadcasted_iota(jnp.int32, (512, 128), 0)
    rows = lax.broadcasted_iota(jnp.int32, (512, 128), 1)
    expert = experts_of_slots(slots, z, x)
    named = (routes_ref[0:1, :] == expert) | (routes_ref[1:2, :] == expert)
    before_r = lax.broadcasted_iota(jnp.int32, (128, 128), 0)
    before_c = lax.broadcasted_iota(jnp.int32, (128, 128), 1)
    same = (before_r >> 6) == (before_c >> 6)
    upper = to_bf16((before_r < before_c) & same)
    lower = to_bf16((before_c < before_r) & same)
    rank = jnp.dot(to_bf16(named), upper, preferred_element_type=jnp.float32)
    wanted = ((slots & 31) - ((rows >> 6) << 4)).astype(jnp.float32)
    pick_v[...] = to_bf16(named & (rank == wanted))
    slots_t = lax.broadcasted_iota(jnp.int32, (128, 512), 1)
    rows_t = lax.broadcasted_iota(jnp.int32, (128, 512), 0)
    expert_t = experts_of_slots(slots_t, z, x).astype(jnp.float32)

    def column(row):
        return jnp.sum(jnp.where(before_r == before_c, row, 0.0), axis=-1, keepdims=True)

    first = column(routes_ref[0:1, :].astype(jnp.float32)) == expert_t
    second = column(routes_ref[1:2, :].astype(jnp.float32)) == expert_t
    rank_t = jnp.dot(lower, to_bf16(first | second), preferred_element_type=jnp.float32)
    here = rank_t == ((slots_t & 31) - ((rows_t >> 6) << 4)).astype(jnp.float32)
    take_v[0] = to_bf16(first & here)
    take_v[1] = to_bf16(second & here)

    for off in range(4):
        for dx in (1, 3, 2):
            slot = kv_all.at[((x - dx + 4) % 4) * 4 + (z - off + 4) % 4]
            remote(slot, slot, k2_s.at[off, dx], k2_r.at[off, dx], device("x", dx)).wait_recv()

    for p in range(3):
        for off in (1, 3, 2):
            phase_copy(p, 1, off, False).wait_recv()
        for off in (1, 3):
            start(phase_copy(p, 2, off, True))
        start(across(p, 0, True))

    keys = kv_all[:, 0].reshape(2048, 128)
    vals = kv_all[:, 1].reshape(2048, 128)
    factor = 128 ** -0.5 * math.log2(math.e)

    def attend(source, target):
        for half in range(2):
            query = q_all[source, pl.ds(half * 2, 2)].reshape(256, 128)
            scores = lax.dot_general(
                query, keys, (((1,), (1,)), ((), ())), preferred_element_type=jnp.float32
            )
            top = jnp.max(scores, axis=-1, keepdims=True)
            power = jnp.exp2((scores - top) * factor)
            share = (power * (1.0 / jnp.sum(power, axis=-1, keepdims=True))).astype(jnp.bfloat16)
            mixed = jnp.dot(share, vals, preferred_element_type=jnp.float32).astype(jnp.bfloat16)
            target[pl.ds(half * 2, 2)] = mixed.reshape(2, 128, 128)

    for off in (2, 1, 3):
        source = (z - off + 4) % 4
        slot = q_all.at[source]
        remote(slot, slot, q_s.at[off], q_r.at[off], device("z", off)).wait_recv()
        attend(source, o_send.at[source])
        start(remote(o_send.at[source], o_all.at[z], o_s.at[off], o_r.at[off], device("z", -off)))
    attend(z, o_all.at[z])

    for p in (1, 2, 0):
        for side, off in ((0, 1), (1, 3)):
            phase_copy(p, 2, off, False).wait_recv()
            start(half_copy(p, side, True))
            start(across(p, 1 + side, True))
    for p in (1, 2, 0):
        for side in (0, 1):
            half_copy(p, side, False).wait_recv()
            start(across(p, 3 + side, True))
    for off in (2, 1, 3):
        slot = o_all.at[(z + off) % 4]
        remote(slot, slot, o_s.at[off], o_r.at[off], device("z", off)).wait_recv()
    for h in range(16):
        att_v[:, h * 128:h * 128 + 128] = o_all[h // 4, h % 4]
    for p in range(3):
        for part in range(5):
            across(p, part, False).wait_recv()
    loads[6].wait()
    for c in range(2):
        for b in range(4):
            first = (b * 2 + c) * 256
            cols = slice(first, first + 256)
            summed = jnp.dot(
                att_v[...], w_all[c, b].reshape(2048, 256), preferred_element_type=jnp.float32
            )
            mixed_ref[:, cols] = residual_v[:, cols].astype(jnp.float32) + summed

    mixed = mixed_ref[...]
    scale = lax.rsqrt(jnp.mean(mixed * mixed, axis=-1, keepdims=True) + EPS)
    normed = (mixed * scale * norm_gain_ref[...]).astype(jnp.bfloat16)

    def exchange(i, src, dst, ssem, rsem, dz, dx):
        return pltpu.make_async_remote_copy(
            src_ref=src.at[pl.ds(i * 32, 32)],
            dst_ref=dst.at[pl.ds(i * 32, 32)],
            send_sem=ssem.at[i],
            recv_sem=rsem.at[i],
            device_id={"sp": peer_of(z, x, dz, dx)},
            device_id_type=MESH,
        )

    outgoing = []
    for i in range(1, 16):
        dz, dx = offset_of(i)
        outgoing.append(exchange(i, send_v, recv_v, ds_sem, dr_sem, dz, dx))
    for c in range(2):
        part = slice(c * 256, c * 256 + 256)
        for n in range(4):
            cols = slice(n * 512, n * 512 + 512)
            sent = jnp.dot(
                pick_v[part], normed[:, cols], preferred_element_type=jnp.float32
            ).astype(jnp.bfloat16)
            send_v[part, cols] = sent
            if c == 0:
                recv_v[0:32, cols] = sent[0:32]
        for i in range(max(1, c * 8), c * 8 + 8):
            outgoing[i - 1].start()


    returning = []
    for i in range(1, 16):
        dz, dx = offset_of(i)
        returning.append(exchange(i, res_v, ret_v, rs_sem, rr_sem, -dz, -dx))
    loads[10].wait()
    loads[11].wait()
    for c in range(2):
        for i in range(max(1, c * 8), c * 8 + 8):
            outgoing[i - 1].wait_recv()
        part = slice(c * 256, c * 256 + 256)
        for n in range(7):
            cols = slice(n * 256, n * 256 + 256)
            gate = jnp.dot(recv_v[part], gate_v[:, cols], preferred_element_type=jnp.float32)
            up = jnp.dot(recv_v[part], up_v[:, cols], preferred_element_type=jnp.float32)
            hid_v[:, cols] = (gate / (1.0 + jnp.exp(-gate)) * up).astype(jnp.bfloat16)
        if c == 0:
            loads[12].wait()
        for n in range(8):
            cols = slice(n * 256, n * 256 + 256)
            done = jnp.dot(
                hid_v[...], down_v[:, cols], preferred_element_type=jnp.float32
            ).astype(jnp.bfloat16)
            res_v[part, cols] = done
            if c == 0:
                ret_v[0:32, cols] = done[0:32]
        for i in range(max(1, c * 8), c * 8 + 8):
            returning[i - 1].start()
    for back in returning:
        back.wait_recv()
    shares = [column(share_ref[k:k + 1, :]) for k in range(2)]
    writes = []
    for n in range(4):
        cols = slice(n * 512, n * 512 + 512)
        got = ret_v[:, cols]
        one = jnp.dot(take_v[0], got, preferred_element_type=jnp.float32)
        two = jnp.dot(take_v[1], got, preferred_element_type=jnp.float32)
        total = mixed_ref[:, cols] + (one * shares[0] + two * shares[1])
        out_v[:, cols] = total.astype(jnp.bfloat16)
        writes.append(pltpu.make_async_copy(out_v.at[:, cols], out_hbm.at[:, cols], local_sem.at[13 + n]))
        writes[-1].start()
    for copy in started + outgoing + returning:
        copy.wait_send()
    for write in writes:
        write.wait()


def layer(
    queries, key_rows, values, query_gain, key_gain, out_weight, residual, norm_gain,
    gate, up, down, routes, route_weight,
):
    dma = pltpu.SemaphoreType.DMA

    def bf16(*shape):
        return pltpu.VMEM(shape, jnp.bfloat16)

    def f32(*shape):
        return pltpu.VMEM(shape, jnp.float32)

    heads = bf16(4, 4, 128, 128)
    rows = bf16(512, 2048)
    return pl.pallas_call(
        layer_kernel,
        out_shape=jax.ShapeDtypeStruct((128, 2048), jnp.bfloat16),
        in_specs=[pl.BlockSpec(memory_space=pl.ANY)] * 13,
        out_specs=pl.BlockSpec(memory_space=pl.ANY),
        scratch_shapes=[
            bf16(128, 16, 128), bf16(128, 4, 128), bf16(128, 4, 128), f32(1, 128), f32(1, 128),
            f32(1, 2048), pltpu.VMEM((2, 128), jnp.int32), f32(2, 128),
            f32(128, 4, 128), f32(128, 4, 128), f32(2048, 128), heads, heads,
            bf16(4, 2, 128, 128), bf16(16, 2, 128, 128), heads, heads,
            bf16(128, 2048), bf16(2, 4, 4, 4, 128, 256), bf16(128, 2048),
            f32(128, 2048), bf16(512, 128), bf16(2, 128, 512),
            bf16(2048, 1792), bf16(2048, 1792), bf16(1792, 2048),
            rows, rows, rows, rows, bf16(256, 1792), bf16(128, 2048),
            dma((17,)),
            dma((4,)), dma((4,)), dma((4, 4)), dma((4, 4)),
            dma((4,)), dma((4,)), dma((4,)), dma((4,)),
            dma((3, 3, 4)), dma((3, 3, 4)), dma((3, 5)), dma((3, 5)),
            dma((16,)), dma((16,)), dma((16,)), dma((16,)),
        ],
        compiler_params=pltpu.CompilerParams(
            collective_id=0, has_side_effects=True, vmem_limit_bytes=63 << 20
        ),
        name="layer",
    )(
        queries, key_rows, values, query_gain.reshape(1, -1), key_gain.reshape(1, -1), out_weight,
        residual, norm_gain.reshape(1, -1), gate, up, down, routes.T, route_weight.T,
    )


def on_device(
    queries,
    key_rows,
    values,
    query_gain,
    key_gain,
    out_weight,
    residual,
    norm_gain,
    expert_gate,
    expert_up,
    expert_down,
    routes,
    route_weight,
):
    return layer(
        queries[0], key_rows[0], values[0], query_gain, key_gain, out_weight, residual[0], norm_gain,
        expert_gate[0], expert_up[0], expert_down[0], routes[0], route_weight[0],
    )[None]


def solution(mesh):
    in_specs = (
        P("dp", "sp", None, None),
        P("dp", "sp", None, None),
        P("dp", "sp", None, None),
        P(),
        P(),
        P("sp", "dp"),
        P("dp", "sp", None),
        P(),
        P("sp", None, None),
        P("sp", None, None),
        P("sp", None, None),
        P("dp", "sp", None),
        P("dp", "sp", None),
    )
    out_specs = P("dp", "sp", None)
    return jax.shard_map(
        on_device, mesh=mesh, in_specs=in_specs, out_specs=out_specs, check_vma=False
    )
```

```python
import math

import jax
import jax.numpy as jnp
from jax import lax
from jax.experimental import pallas as pl
from jax.experimental.pallas import tpu as pltpu
from jax.sharding import PartitionSpec as P

MESH = pl.DeviceIdType.MESH
EPS = 1e-06
THETA = 10000.0
PIECES = (
    ((0, 64), ("x", "z", "y")),
    ((64, 96), ("y", "x", "z")),
    ((96, 128), ("y", "z", "x")),
)
AXES = ("y", "z", "x")


TURN = (0, 1, 3, 2)


def sent_row(blk, first, second):
    return blk * 256 + first * 64 + second * 16


def held_row(blk, first, second):
    return TURN.index(first) * 128 + blk * 64 + second * 16


def relay_row(blk, first, second):
    return (blk * 3 + first - 1) * 48 + (second - 1) * 16


def peer_of(z, x, dz, dx):
    return ((z + dz) % 4) * 4 + (x + dx) % 4


def experts_of_slots(slots, z, x):
    first, second, other = (slots >> 6) & 3, (slots >> 4) & 3, slots >= 256
    dz = jnp.where(other, first, second)
    dx = jnp.where(other, second, first)
    return (((z + dz) & 3) << 2) | ((x + dx) & 3)


def to_bf16(mask):
    return jnp.where(mask, 1.0, 0.0).astype(jnp.bfloat16)


def layer_kernel(
    q_hbm, k_hbm, v_hbm, q_gain_hbm, k_gain_hbm, weight_hbm, residual_hbm, norm_gain_hbm,
    gate_hbm, up_hbm, down_hbm, routes_hbm, share_hbm,
    out_v,
    q_raw, k_raw, v_raw, q_gain_ref, k_gain_ref, norm_gain_ref, routes_ref, share_ref,
    k_f32, v_f32, q_f32, q_send, q_all, kv_send, kv_all, o_send, o_all, att_v, w_all, residual_v,
    mixed_ref, pick_v, take_v,
    gate_v, up_v, down_v, send_v, mid_v, recv_v, res_v, rmid_v, ret_v, hid_v,
    local_sem, k1_s, k1_r, k2_s, k2_r, q_s, q_r, o_s, o_r, w_s, w_r, u_s, u_r, p_s, p_r,
    m_s, m_r, d_s, d_r, n_s, n_r, b_s, b_r,
):
    me = lax.axis_index("sp")
    dp = lax.axis_index("dp")
    at = {"z": me // 4, "x": me % 4, "y": dp // 2}
    z, x, y, core = at["z"], at["x"], at["y"], dp % 2

    def device(axis, off):
        if axis == "core":
            return {"dp": y * 2 + (1 - core)}
        v = (at[axis] + off + 4) % 4
        if axis == "y":
            return {"dp": v * 2 + core}
        return {"sp": v * 4 + x if axis == "z" else z * 4 + v}

    def remote(src, dst, ssem, rsem, target):
        return pltpu.make_async_remote_copy(
            src_ref=src, dst_ref=dst, send_sem=ssem, recv_sem=rsem,
            device_id=target, device_id_type=MESH,
        )

    def piece_ref(p, gathered, axis, value, cols=None, owner=None, unit=None):
        rows = pl.ds(PIECES[p][0][0], PIECES[p][0][1] - PIECES[p][0][0])
        index = [core if owner is None else owner]
        for name in AXES:
            if name == axis:
                index.append(value)
            elif name == "z" and unit is not None:
                index.append((z - unit + 4) % 4)
            else:
                index.append(slice(None) if name in gathered else at[name])
        index += [rows, slice(None) if cols is None else cols]
        return w_all.at[tuple(index)]

    barrier = pltpu.get_barrier_semaphore()
    for i in range(1, 16):
        pl.semaphore_signal(
            barrier, inc=1, device_id={"sp": peer_of(z, x, i // 4, i % 4)}, device_id_type=MESH
        )
    for off in (1, 2, 3):
        pl.semaphore_signal(barrier, inc=1, device_id=device("y", off), device_id_type=MESH)
    pl.semaphore_signal(barrier, inc=1, device_id=device("core", 1), device_id_type=MESH)
    loads = [
        pltpu.make_async_copy(src, dst, local_sem.at[n])
        for n, (src, dst) in enumerate(
            (
                (k_hbm, k_raw), (v_hbm, v_raw), (k_gain_hbm, k_gain_ref), (q_gain_hbm, q_gain_ref),
                (q_hbm, q_raw), (weight_hbm, w_all.at[core, y, z, x]), (residual_hbm, residual_v),
                (norm_gain_hbm, norm_gain_ref), (routes_hbm, routes_ref), (share_hbm, share_ref),
                (gate_hbm, gate_v), (up_hbm, up_v), (down_hbm, down_v),
            )
        )
    ]
    for load in loads:
        load.start()

    lane = lax.broadcasted_iota(jnp.int32, (128, 128), 1)
    position = lax.broadcasted_iota(jnp.int32, (128, 128), 0) + me * 128
    place = jnp.where(lane < 64, position >> 6, position & 63).astype(jnp.float32)
    rate = jnp.exp((lane & 31).astype(jnp.float32) * (-math.log(THETA) / 32))
    angle = place * rate
    cosine = jnp.cos(angle)
    low = (lane & 63) < 32
    sine = jnp.where(low, -jnp.sin(angle), jnp.sin(angle))

    def turned(rows, gain):
        scaled = rows * lax.rsqrt(jnp.mean(rows * rows, axis=-1, keepdims=True) + EPS) * gain
        other = jnp.where(low, pltpu.roll(scaled, 96, 1), pltpu.roll(scaled, 32, 1))
        return (scaled * cosine + other * sine).astype(jnp.bfloat16)

    for load in loads[:4]:
        load.wait()
    k_f32[...] = k_raw[...].astype(jnp.float32)
    v_f32[...] = v_raw[...].astype(jnp.float32)
    for h in range(4):
        kv_send[h, 0] = turned(k_f32[:, h, :], k_gain_ref[...])
        kv_send[h, 1] = v_f32[:, h, :].astype(jnp.bfloat16)
    kv_all[x * 4 + z] = kv_send[z]
    loads[4].wait()
    q_f32[...] = q_raw[...].reshape(2048, 128).astype(jnp.float32)
    pl.semaphore_wait(barrier, 19)

    started = []

    def start(copy):
        copy.start()
        started.append(copy)

    def phase_copy(p, n, off, outgoing, unit=None):
        order = PIECES[p][1]
        gathered, axis = order[:n], order[n]
        value = at[axis] if outgoing else (at[axis] - off + 4) % 4
        block = piece_ref(p, gathered, axis, value, unit=unit)
        sems = (w_s.at[p, n, off], w_r.at[p, n, off])
        if unit is not None:
            sems = (u_s.at[unit, off], u_r.at[unit, off])
        return remote(block, block, *sems, device(axis, off))

    def half_copy(p, side, outgoing, unit=None):
        order = PIECES[p][1]
        axis = order[2]
        step = 1 if side == 0 else 3
        value = (at[axis] - step + 4) % 4 if outgoing else (at[axis] + 2) % 4
        block = piece_ref(p, order[:2], axis, value, cols=pl.ds(side * 128, 128), unit=unit)
        n = 2 if side == 0 else 0
        sems = (w_s.at[p, 2, n], w_r.at[p, 2, n])
        if unit is not None:
            sems = (u_s.at[unit, n], u_r.at[unit, n])
        return remote(block, block, *sems, device(axis, step))

    def across(p, part, outgoing):
        order = PIECES[p][1]
        axis = order[2]
        owner = core if outgoing else 1 - core
        cols = None
        if part == 0:
            value = at[axis]
        elif part < 3:
            value = (at[axis] - (1, 3)[part - 1] + 4) % 4
        else:
            value = (at[axis] + 2) % 4
            cols = pl.ds((part - 3) * 128, 128)
        block = piece_ref(p, order[:2], axis, value, cols=cols, owner=owner)
        return remote(block, block, p_s.at[p, part], p_r.at[p, part], device("core", 1))

    def ring_out(p, unit=None):
        for off in (1, 3):
            start(phase_copy(p, 2, off, True, unit))

    def ring_on(p, unit=None):
        for side, off in ((0, 1), (1, 3)):
            phase_copy(p, 2, off, False, unit).wait_recv()
            start(half_copy(p, side, True, unit))

    loads[5].wait()
    for p in range(3):
        for off in (1, 3, 2):
            start(phase_copy(p, 0, off, True))

    def kv_in(off):
        return remote(kv_send.at[(z + off) % 4], kv_all.at[x * 4 + z], k1_s.at[off], k1_r.at[off], device("z", off))

    def spread(off):
        slot = kv_all.at[x * 4 + (z - off + 4) % 4]
        for dx in (1, 3, 2):
            start(remote(slot, slot, k2_s.at[off, dx], k2_r.at[off, dx], device("x", dx)))

    for off in (1, 3, 2):
        start(kv_in(off))
    spread(0)

    for h in range(16):
        q_send[h // 4, h % 4] = turned(q_f32[pl.ds(h, 128, stride=16), :], q_gain_ref[...])
    q_all[z] = q_send[z]
    for off in (2, 1, 3):
        start(remote(q_send.at[(z + off) % 4], q_all.at[z], q_s.at[off], q_r.at[off], device("z", off)))

    for off in (1, 3, 2):
        phase_copy(0, 0, off, False).wait_recv()
    ring_out(0, 0)
    for off in (1, 3, 2):
        start(phase_copy(0, 1, off, True))

    for off in (1, 3, 2):
        incoming = kv_all.at[x * 4 + (z - off + 4) % 4]
        remote(incoming, incoming, k1_s.at[off], k1_r.at[off], device("z", off)).wait_recv()
        spread(off)

    for p in (1, 2):
        for off in (1, 3, 2):
            phase_copy(p, 0, off, False).wait_recv()
        for off in (1, 3, 2):
            start(phase_copy(p, 1, off, True))

    for load in loads[7:10]:
        load.wait()
    slots = lax.broadcasted_iota(jnp.int32, (512, 128), 0)
    rows = lax.broadcasted_iota(jnp.int32, (512, 128), 1)
    expert = experts_of_slots(slots, z, x)
    named = (routes_ref[0:1, :] == expert) | (routes_ref[1:2, :] == expert)
    before_r = lax.broadcasted_iota(jnp.int32, (128, 128), 0)
    before_c = lax.broadcasted_iota(jnp.int32, (128, 128), 1)
    same = (before_r >> 6) == (before_c >> 6)
    upper = to_bf16((before_r < before_c) & same)
    lower = to_bf16((before_c < before_r) & same)
    rank = jnp.dot(to_bf16(named), upper, preferred_element_type=jnp.float32)
    wanted = (slots & 15).astype(jnp.float32)
    pick_v[...] = to_bf16(named & (rank == wanted) & ((rows >> 6) == (slots >> 8)))
    slots_t = lax.broadcasted_iota(jnp.int32, (128, 512), 1)
    rows_t = lax.broadcasted_iota(jnp.int32, (128, 512), 0)
    expert_t = experts_of_slots(slots_t, z, x).astype(jnp.float32)

    def column(row):
        return jnp.sum(jnp.where(before_r == before_c, row, 0.0), axis=-1, keepdims=True)

    first = column(routes_ref[0:1, :].astype(jnp.float32)) == expert_t
    second = column(routes_ref[1:2, :].astype(jnp.float32)) == expert_t
    rank_t = jnp.dot(lower, to_bf16(first | second), preferred_element_type=jnp.float32)
    here = (rank_t == (slots_t & 15).astype(jnp.float32)) & ((rows_t >> 6) == (slots_t >> 8))
    take_v[0] = to_bf16(first & here)
    take_v[1] = to_bf16(second & here)

    def row_in(off):
        phase_copy(0, 1, off, False).wait_recv()
        ring_out(0, off)

    def plane_in(p):
        for off in (1, 3, 2):
            phase_copy(p, 1, off, False).wait_recv()
        ring_out(p)
        start(across(p, 0, True))

    row_in(1)
    row_in(3)
    plane_in(1)
    plane_in(2)
    ring_on(0, 0)
    row_in(2)
    start(across(0, 0, True))
    for off in range(4):
        for dx in (1, 3, 2):
            slot = kv_all.at[((x - dx + 4) % 4) * 4 + (z - off + 4) % 4]
            remote(slot, slot, k2_s.at[off, dx], k2_r.at[off, dx], device("x", dx)).wait_recv()

    keys = kv_all[:, 0].reshape(2048, 128)
    vals = kv_all[:, 1].reshape(2048, 128)
    factor = 128 ** -0.5 * math.log2(math.e)

    def attend(source, target):
        for half in range(2):
            query = q_all[source, pl.ds(half * 2, 2)].reshape(256, 128)
            scores = lax.dot_general(
                query, keys, (((1,), (1,)), ((), ())), preferred_element_type=jnp.float32
            )
            top = jnp.max(scores, axis=-1, keepdims=True)
            power = jnp.exp2((scores - top) * factor)
            total = jnp.sum(power, axis=-1, keepdims=True)
            mixed = jnp.dot(power.astype(jnp.bfloat16), vals, preferred_element_type=jnp.float32)
            target[pl.ds(half * 2, 2)] = (mixed / total).astype(jnp.bfloat16).reshape(2, 128, 128)

    def attend_to(off):
        source = (z - off + 4) % 4
        slot = q_all.at[source]
        remote(slot, slot, q_s.at[off], q_r.at[off], device("z", off)).wait_recv()
        attend(source, o_send.at[source])
        start(remote(o_send.at[source], o_all.at[z], o_s.at[off], o_r.at[off], device("z", -off)))

    attend_to(2)
    ring_on(0, 1)
    ring_on(0, 3)
    attend_to(1)
    ring_on(0, 2)
    start(across(0, 1, True))
    start(across(0, 2, True))
    attend_to(3)
    for p in (1, 2):
        ring_on(p)
        start(across(p, 1, True))
        start(across(p, 2, True))
    attend(z, o_all.at[z])
    for side in (0, 1):
        for p in (1, 2):
            half_copy(p, side, False).wait_recv()
            start(across(p, 3 + side, True))
        for unit in (0, 1, 3, 2):
            half_copy(0, side, False, unit).wait_recv()
        start(across(0, 3 + side, True))
    for off in (2, 1, 3):
        slot = o_all.at[(z + off) % 4]
        remote(slot, slot, o_s.at[off], o_r.at[off], device("z", off)).wait_recv()
    for h in range(16):
        att_v[:, h * 128:h * 128 + 128] = o_all[h // 4, h % 4]
    loads[6].wait()

    def project(c):
        for b in range(4):
            cols = pl.ds(pl.multiple_of((b * 2 + c) * 256, 256), 256)
            summed = jnp.dot(
                att_v[...], w_all[c, b].reshape(2048, 256), preferred_element_type=jnp.float32
            )
            mixed_ref[:, cols] = residual_v[:, cols].astype(jnp.float32) + summed

    project(core)
    for p in range(3):
        for part in range(5):
            across(p, part, False).wait_recv()
    project(1 - core)

    mixed = mixed_ref[...]
    scale = lax.rsqrt(jnp.mean(mixed * mixed, axis=-1, keepdims=True) + EPS)
    normed = (mixed * scale * norm_gain_ref[...]).astype(jnp.bfloat16)

    def line(blk, second):
        return ("x", "z")[blk != second]

    def piece(ref, row, count=16):
        return ref.at[pl.ds(row, count)]

    def to_relay(blk, first):
        return remote(
            piece(send_v, sent_row(blk, first, 1), 48), piece(mid_v, relay_row(blk, first, 1), 48),
            m_s.at[blk, first], m_r.at[blk, first], device(line(blk, 0), first),
        )

    def to_expert(blk, first, second):
        dst = piece(recv_v, held_row(blk, first, second))
        if second == 0:
            src, target = piece(send_v, sent_row(blk, first, 0)), device(line(blk, 0), first)
        else:
            src = piece(send_v, sent_row(blk, 0, second))
            if first > 0:
                src = piece(mid_v, relay_row(blk, first, second))
            target = device(line(blk, 1), second)
        return remote(src, dst, d_s.at[blk, first, second], d_r.at[blk, first, second], target)

    def back_relay(blk, first, second):
        return remote(
            piece(res_v, held_row(blk, first, second)), piece(rmid_v, relay_row(blk, first, second)),
            n_s.at[blk, first, second], n_r.at[blk, first, second], device(line(blk, 1), -second),
        )

    def back_home(blk, first, second):
        if first > 0 and second > 0:
            src = piece(rmid_v, relay_row(blk, first, second))
        else:
            src = piece(res_v, held_row(blk, first, second))
        target = device(line(blk, 0), -first) if first > 0 else device(line(blk, 1), -second)
        return remote(
            src, piece(ret_v, sent_row(blk, first, second)),
            b_s.at[blk, first, second], b_r.at[blk, first, second], target,
        )

    for blk in range(2):
        part = slice(blk * 256, blk * 256 + 256)
        own, home = held_row(blk, 0, 0), sent_row(blk, 0, 0)
        for n in range(4):
            cols = slice(n * 512, n * 512 + 512)
            sent = jnp.dot(
                pick_v[part], normed[:, cols], preferred_element_type=jnp.float32
            ).astype(jnp.bfloat16)
            send_v[part, cols] = sent
            recv_v[own:own + 16, cols] = sent[0:16]
    for first in (1, 3):
        for blk in range(2):
            start(to_relay(blk, first))
    for blk in range(2):
        for second in (1, 3):
            start(to_expert(blk, 0, second))
    for blk in range(2):
        start(to_expert(blk, 1, 0))
        start(to_expert(blk, 0, 2))

    def relay(first):
        for blk in range(2):
            to_relay(blk, first).wait_recv()
            for second in (1, 3, 2):
                start(to_expert(blk, first, second))

    relay(1)
    for blk in range(2):
        start(to_relay(blk, 2))
        start(to_expert(blk, 3, 0))
        start(to_expert(blk, 2, 0))
    loads[10].wait()
    loads[11].wait()
    loads[12].wait()

    def forward(firsts, seconds):
        for second in seconds:
            for blk in range(2):
                for first in firsts:
                    back_relay(blk, first, second).wait_recv()
                    start(back_home(blk, first, second))

    for c in range(4):
        firsts = TURN[c:c + 1]
        part = slice(c * 128, c * 128 + 128)
        if c == 3:
            forward((1,), (1, 3))
        for first in firsts:
            for blk in range(2):
                for second in range(4):
                    if first > 0 or second > 0:
                        to_expert(blk, first, second).wait_recv()
        for n in range(7):
            cols = slice(n * 256, n * 256 + 256)
            gate = jnp.dot(recv_v[part], gate_v[:, cols], preferred_element_type=jnp.float32)
            up = jnp.dot(recv_v[part], up_v[:, cols], preferred_element_type=jnp.float32)
            hid_v[:, cols] = (gate / (1.0 + jnp.exp(-gate)) * up).astype(jnp.bfloat16)
        if c == 0:
            relay(3)
        elif c == 1:
            relay(2)
        elif c == 3:
            forward((1,), (2,))
            forward((3,), (1, 3))
        for n in range(8):
            cols = slice(n * 256, n * 256 + 256)
            done = jnp.dot(
                hid_v[...], down_v[:, cols], preferred_element_type=jnp.float32
            ).astype(jnp.bfloat16)
            res_v[part, cols] = done
            if c == 0:
                for blk in range(2):
                    own, home = held_row(blk, 0, 0), sent_row(blk, 0, 0)
                    ret_v[home:home + 16, cols] = done[own:own + 16]
        for second in (1, 3, 2):
            for blk in range(2):
                for first in firsts:
                    start((back_relay if first > 0 else back_home)(blk, first, second))
        for first in firsts:
            for blk in range(2):
                if first > 0:
                    start(back_home(blk, first, 0))
    forward((3,), (2,))
    forward((2,), (1, 3, 2))
    for first in range(4):
        for blk in range(2):
            for second in range(4):
                if first > 0 or second > 0:
                    back_home(blk, first, second).wait_recv()
    shares = [column(share_ref[k:k + 1, :]) for k in range(2)]
    for n in range(4):
        cols = slice(n * 512, n * 512 + 512)
        got = ret_v[:, cols]
        one = jnp.dot(take_v[0], got, preferred_element_type=jnp.float32)
        two = jnp.dot(take_v[1], got, preferred_element_type=jnp.float32)
        total = mixed_ref[:, cols] + (one * shares[0] + two * shares[1])
        out_v[:, cols] = total.astype(jnp.bfloat16)
    for copy in started:
        copy.wait_send()


def layer(
    queries, key_rows, values, query_gain, key_gain, out_weight, residual, norm_gain,
    gate, up, down, routes, route_weight,
):
    dma = pltpu.SemaphoreType.DMA

    def bf16(*shape):
        return pltpu.VMEM(shape, jnp.bfloat16)

    def f32(*shape):
        return pltpu.VMEM(shape, jnp.float32)

    heads = bf16(4, 4, 128, 128)
    rows = bf16(512, 2048)
    return pl.pallas_call(
        layer_kernel,
        out_shape=jax.ShapeDtypeStruct((128, 2048), jnp.bfloat16),
        in_specs=[pl.BlockSpec(memory_space=pltpu.HBM)] * 13,
        out_specs=pl.BlockSpec(memory_space=pltpu.VMEM),
        scratch_shapes=[
            bf16(128, 16, 128), bf16(128, 4, 128), bf16(128, 4, 128), f32(1, 128), f32(1, 128),
            f32(1, 2048), pltpu.VMEM((2, 128), jnp.int32), f32(2, 128),
            f32(128, 4, 128), f32(128, 4, 128), f32(2048, 128), heads, heads,
            bf16(4, 2, 128, 128), bf16(16, 2, 128, 128), heads, heads,
            bf16(128, 2048), bf16(2, 4, 4, 4, 128, 256), bf16(128, 2048),
            f32(128, 2048), bf16(512, 128), bf16(2, 128, 512),
            bf16(2048, 1792), bf16(2048, 1792), bf16(1792, 2048),
            rows, bf16(288, 2048), rows, rows, bf16(288, 2048), rows, bf16(128, 1792),
            dma((13,)),
            dma((4,)), dma((4,)), dma((4, 4)), dma((4, 4)),
            dma((4,)), dma((4,)), dma((4,)), dma((4,)),
            dma((3, 3, 4)), dma((3, 3, 4)), dma((4, 4)), dma((4, 4)), dma((3, 5)), dma((3, 5)),
            dma((2, 4)), dma((2, 4)), *[dma((2, 4, 4))] * 6,
        ],
        compiler_params=pltpu.CompilerParams(
            collective_id=0, has_side_effects=True, vmem_limit_bytes=58 << 20
        ),
        name="layer",
    )(
        queries, key_rows, values, query_gain.reshape(1, -1), key_gain.reshape(1, -1), out_weight,
        residual, norm_gain.reshape(1, -1), gate, up, down, routes.T, route_weight.T,
    )


def on_device(
    queries,
    key_rows,
    values,
    query_gain,
    key_gain,
    out_weight,
    residual,
    norm_gain,
    expert_gate,
    expert_up,
    expert_down,
    routes,
    route_weight,
):
    return layer(
        queries[0], key_rows[0], values[0], query_gain, key_gain, out_weight, residual[0], norm_gain,
        expert_gate[0], expert_up[0], expert_down[0], routes[0], route_weight[0],
    )[None]


def solution(mesh):
    in_specs = (
        P("dp", "sp", None, None),
        P("dp", "sp", None, None),
        P("dp", "sp", None, None),
        P(),
        P(),
        P("sp", "dp"),
        P("dp", "sp", None),
        P(),
        P("sp", None, None),
        P("sp", None, None),
        P("sp", None, None),
        P("dp", "sp", None),
        P("dp", "sp", None),
    )
    out_specs = P("dp", "sp", None)
    return jax.shard_map(
        on_device, mesh=mesh, in_specs=in_specs, out_specs=out_specs, check_vma=False
    )
```
